32 devices in a mesh: ra: 8 (over z, y), cb: 4 (over x, core).
Axes of the slice: x: 2, y: 2, z: 4, core: 2. Of those that a mesh axis runs over, the one named last changes fastest.
Arguments:
- tokens: bfloat16 [512, 4096], P(None, 'cb'), may hold values from -400 to 400
- norm_gain: bfloat16 [4096], P('cb'), may hold values from 0.099609375 to 1.8984375
- w_gate: bfloat16 [4096, 11264], P('cb', 'ra'), may hold values from -0.09375 to 0.09375
- w_up: bfloat16 [4096, 11264], P('cb', 'ra'), may hold values from -0.09375 to 0.09375
- w_down: bfloat16 [11264, 4096], P('ra', 'cb'), may hold values from -0.0546875 to 0.0546875
- out_gain: bfloat16 [4096], P('cb'), may hold values from 0.099609375 to 1.8984375
Outputs:
- normed_out: bfloat16 [512, 4096], P('ra', 'cb')
The draws below stay inside these ranges and needn't reach their ends.
All inputs are finite; a program needn't handle non-finite values.
Results may differ from the reference program's by a relative error of at most 0.0045.
Values sent between devices are 32-bit elements; how exact they have to be, the bound alone decides.
A program may use at most 64 MiB of HBM per device.

```python
import jax
import jax.numpy as jnp
from jax import lax

D = 4096
FF = 11264
TOKENS = 512


def draw_tokens(key, part):
    first, second, third = jax.random.split(jax.random.fold_in(key, 17), 3)
    rise = jnp.arange(D, dtype=jnp.float32) / D
    jitter = jax.random.uniform(second, (D,), jnp.float32)
    column_scale = jnp.exp(jnp.log(10.0) * (0.8 * rise + 0.2 * jitter))
    row_scale = jnp.exp(jnp.log(10.0) * jax.random.uniform(third, (TOKENS, 1), jnp.float32))
    base = jnp.clip(jax.random.normal(first, (TOKENS, D), jnp.float32), -4.0, 4.0)
    return (base * row_scale * column_scale[None, :]).astype(jnp.bfloat16)


def level_of(stream_key, dims, cuts, least, largest):
    gain, own = 1.0, jax.random.fold_in(stream_key, 6)
    for dim, parts in cuts:
        draws = jnp.exp(jax.random.uniform(jax.random.fold_in(own, dim), (parts,), jnp.float32, least / len(cuts), largest / len(cuts)))
        gain = gain * jnp.repeat(draws, dims[dim] // parts).reshape([-1 if axis == dim else 1 for axis in range(len(dims))])
    return gain


def scatter_about(rng, shape, deviation, most, shards=(), held_as=jnp.bfloat16):
    loudness = level_of(rng, shape, shards, -0.22, 0.18) if shards else 1.0
    drawn = jax.random.normal(rng, shape, jnp.float32) * deviation * loudness
    return jnp.minimum(jnp.maximum(drawn, -most), most).astype(held_as)


def setup_inputs(seed: int = 0) -> dict:
    keys = jax.random.split(jax.random.key(seed), 7)
    return {
        "tokens": draw_tokens(jax.random.fold_in(keys[6], 71), 0),
        "norm_gain": jnp.clip(1.0 + 0.18 * jax.random.normal(keys[1], (D,), jnp.float32), 0.099609375, 1.8984375).astype(jnp.bfloat16),
        "w_gate": scatter_about(keys[2], (D, FF), D ** -0.5, 0.09375, ((0, 4), (1, 8))),
        "w_up": scatter_about(keys[3], (D, FF), D ** -0.5, 0.09375, ((0, 4), (1, 8))),
        "w_down": scatter_about(keys[4], (FF, D), FF ** -0.5, 0.0546875, ((0, 8), (1, 4))),
        "out_gain": jnp.clip(1.0 + 0.18 * jax.random.normal(keys[5], (D,), jnp.float32), 0.099609375, 1.8984375).astype(jnp.bfloat16),
    }


def reference(tokens, norm_gain, w_gate, w_up, w_down, out_gain):
    eps = 1e-06
    xfloat = tokens.astype(jnp.float32)
    inv_in = lax.rsqrt(lax.optimization_barrier(jnp.mean(xfloat * xfloat, axis=1, keepdims=True)) + eps)
    scaled = (xfloat * norm_gain.astype(jnp.float32)).astype(jnp.bfloat16)
    gate = jnp.dot(scaled, w_gate, preferred_element_type=jnp.float32) * inv_in
    up = jnp.dot(scaled, w_up, preferred_element_type=jnp.float32) * inv_in
    hidden = (jax.nn.silu(gate) * up).astype(jnp.bfloat16)
    down = jnp.dot(hidden, w_down, preferred_element_type=jnp.float32)
    mixed = 0.1 * xfloat + down
    inv_out = lax.rsqrt(lax.optimization_barrier(jnp.mean(mixed * mixed, axis=1, keepdims=True)) + eps)
    return (mixed * inv_out * out_gain.astype(jnp.float32)).astype(jnp.bfloat16)
```

```python
import functools

import jax
import jax.numpy as jnp
from jax import lax
from jax.experimental import pallas as pl
from jax.experimental.pallas import tpu as pltpu
from jax.sharding import PartitionSpec as P

EPS = 1e-06
LANES = 128
TILE = 256
CHUNKS = 4
VMEM_BYTES = 64 * 1024 * 1024 - 64 * 1024


def plain_body(width, tokens, norm_gain, w_gate, w_up, w_down, out_gain):
    xfloat = tokens.astype(jnp.float32)
    local_sq = jnp.sum(xfloat * xfloat, axis=1)
    scaled = (xfloat * norm_gain.astype(jnp.float32)).astype(jnp.bfloat16)
    gate_part = jnp.dot(scaled, w_gate, preferred_element_type=jnp.float32)
    up_part = jnp.dot(scaled, w_up, preferred_element_type=jnp.float32)
    total_sq, gate_sum, up_sum = lax.psum((local_sq, gate_part, up_part), "cb")
    inv_in = lax.rsqrt(total_sq / width + EPS)[:, None]
    hidden = (jax.nn.silu(gate_sum * inv_in) * (up_sum * inv_in)).astype(jnp.bfloat16)
    partial_down = jnp.dot(hidden, w_down, preferred_element_type=jnp.float32)
    own_rows = tokens.shape[0] // lax.axis_size("ra")
    first_row = lax.axis_index("ra") * own_rows
    down = lax.psum_scatter(partial_down, "ra", scatter_dimension=0, tiled=True)
    residual = lax.dynamic_slice_in_dim(xfloat, first_row, own_rows, 0)
    mixed = 0.1 * residual + down
    out_sq = lax.psum(jnp.sum(mixed * mixed, axis=1), "cb")
    inv_out = lax.rsqrt(out_sq / width + EPS)[:, None]
    return (mixed * inv_out * out_gain.astype(jnp.float32)).astype(jnp.bfloat16)


def kernel(n_ra, width, tok_hbm, ng_hbm, wg_hbm, wu_hbm, wd_hbm, og_hbm, out_ref,
           tok, rest, ng, og, wgu, wd, xs, xb, mixed,
           part, prec, xrec, sqp, sqd, sqx, hid, dn, yrec, zrec, osq,
           ld, s_d, r_d, s_x, r_x, s_hx, r_hx, s_h1, r_h1, s_h2, r_h2,
           s_y, r_y, s_z, r_z, s_o, r_o, s_q, r_q):
    chunks, rows, depth = xs.shape
    units = wd.shape[0]
    own = rest.shape[0]
    sub = own // chunks
    nz = n_ra // 2
    quarter = rows // 4
    ra, cb = lax.axis_index("ra"), lax.axis_index("cb")
    c, x = lax.rem(cb, 2), lax.div(cb, 2)
    y, z = lax.rem(ra, 2), lax.div(ra, 2)
    oc, ox, oy = 1 - c, 1 - x, 1 - y
    core_peer = (ra, x * 2 + oc)
    x_peer = (ra, ox * 2 + c)
    diag_peer = (ra, ox * 2 + oc)
    y_peer = (z * 2 + oy, cb)
    z_peers = [(lax.rem(z + d, nz) * 2 + y, cb) for d in range(1, nz)]
    mesh_id = pl.DeviceIdType.MESH

    loads = [
        pltpu.make_async_copy(tok_hbm, tok, ld.at[0]),
        pltpu.make_async_copy(ng_hbm, ng, ld.at[1]),
        pltpu.make_async_copy(wg_hbm, wgu.at[:, pl.ds(0, units)], ld.at[2]),
        pltpu.make_async_copy(wu_hbm, wgu.at[:, pl.ds(units, units)], ld.at[3]),
        pltpu.make_async_copy(tok_hbm.at[pl.ds(pl.multiple_of(ra * own, own), own)], rest, ld.at[4]),
        pltpu.make_async_copy(og_hbm, og, ld.at[5]),
        pltpu.make_async_copy(wd_hbm, wd, ld.at[6]),
    ]
    for load in loads:
        load.start()

    barrier = pltpu.get_barrier_semaphore()
    peers = [core_peer, x_peer, diag_peer, y_peer] + z_peers
    for peer in peers:
        pl.semaphore_signal(barrier, inc=1, device_id=peer, device_id_type=mesh_id)

    sends = []

    def send(src, dst, s, r, peer):
        copy = pltpu.make_async_remote_copy(
            src_ref=src, dst_ref=dst, send_sem=s, recv_sem=r,
            device_id=peer, device_id_type=mesh_id)
        copy.start()
        sends.append(copy)
        return copy

    loads[0].wait()
    loads[1].wait()
    lane = lax.broadcasted_iota(jnp.int32, (sub, LANES), 1)
    gain = ng[...].astype(jnp.float32)
    for d in range(n_ra):
        xf = tok[pl.ds(d * own, own), :].astype(jnp.float32)
        sq = jnp.sum(xf * xf, axis=1, keepdims=True)
        sc = xf * gain
        at = (d % 2) * nz * sub + (d // 2) * sub
        total = jnp.zeros((sub, LANES), jnp.float32)
        for k in range(chunks):
            xs[k, pl.ds(at, sub), :] = sc[k * sub:(k + 1) * sub]
            total = total + jnp.where(lane == k, sq[k * sub:(k + 1) * sub], 0.0)
        q, off = at // quarter, at % quarter
        sqp[q // 2, q % 2, pl.ds(off, sub), :] = total
    for k in range(chunks):
        xb[k] = xs[k].astype(jnp.bfloat16)

    def project(k):
        def tile(j, carry):
            cols = pl.ds(pl.multiple_of(j * TILE, TILE), TILE)
            got = jnp.dot(xb[k], wgu[:, cols], preferred_element_type=jnp.float32)
            part[k, :, :, :, cols] = got.reshape(2, 2, quarter, TILE)
            return carry
        lax.fori_loop(0, 2 * units // TILE, tile, 0)
        return send(part.at[k, oc], prec.at[k], s_d.at[k], r_d.at[k], core_peer)

    def combine(k, copy):
        copy.wait_recv()
        def tile(j, carry):
            cols = pl.ds(pl.multiple_of(j * TILE, TILE), TILE)
            part[k, c, :, :, cols] += prec[k, :, :, cols]
            return carry
        lax.fori_loop(0, 2 * units // TILE, tile, 0)
        return send(part.at[k, c, ox], xrec.at[k], s_x.at[k], r_x.at[k], x_peer)

    def activate(k, copy, inv):
        copy.wait_recv()
        scale = inv[:, k:k + 1]
        def tile(j, carry):
            left = pl.ds(pl.multiple_of(j * LANES, LANES), LANES)
            right = pl.ds(pl.multiple_of(units + j * LANES, LANES), LANES)
            gate = (part[k, c, x, :, left] + xrec[k, :, left]) * scale
            up = (part[k, c, x, :, right] + xrec[k, :, right]) * scale
            val = gate / (1.0 + jnp.exp(-gate)) * up
            hid[k, c, x, :, left] = val.astype(jnp.bfloat16).astype(jnp.float32)
            return carry
        lax.fori_loop(0, units // LANES, tile, 0)
        block = hid.at[k, c, x]
        hx = send(block, block, s_hx.at[k], r_hx.at[k], x_peer)
        h1 = send(block, block, s_h1.at[k], r_h1.at[k], core_peer)
        return hx, h1

    def forward(k, hx):
        hx.wait_recv()
        block = hid.at[k, c, ox]
        return send(block, block, s_h2.at[k], r_h2.at[k], core_peer)

    def lower(k, h1, h2):
        h1.wait_recv()
        h2.wait_recv()
        hb = hid[k].reshape(rows, units).astype(jnp.bfloat16)
        for j in range(depth // TILE):
            cols = slice(j * TILE, (j + 1) * TILE)
            got = jnp.dot(hb, wd[:, cols], preferred_element_type=jnp.float32)
            dn[k, :, :, :, cols] = got.reshape(2, nz, sub, TILE)
        return send(dn.at[k, oy], yrec.at[k], s_y.at[k], r_y.at[k], y_peer)

    def across(k, copy):
        copy.wait_recv()
        dn[k, y] += yrec[k]
        return [
            send(dn.at[k, y, lax.rem(z + d, nz)], zrec.at[k, d - 1],
                 s_z.at[k, d - 1], r_z.at[k, d - 1], z_peers[d - 1])
            for d in range(1, nz)]

    def finish(k, copies):
        got = dn[k, y, z]
        for d, copy in enumerate(copies):
            copy.wait_recv()
            got = got + zrec[k, d]
        got = 0.1 * rest[pl.ds(k * sub, sub), :].astype(jnp.float32) + got
        mixed[pl.ds(k * sub, sub), :] = got
        osq[0, k] = jnp.broadcast_to(jnp.sum(got * got, axis=1, keepdims=True), (sub, LANES))
        return [
            send(osq.at[0, k], osq.at[i + 1, k], s_o.at[k, i], r_o.at[k, i], peer)
            for i, peer in enumerate((core_peer, x_peer, diag_peer))]

    pl.semaphore_wait(barrier, len(peers))
    q1 = send(sqp.at[oc], sqd, s_q.at[0], r_q.at[0], core_peer)
    loads[2].wait()
    loads[3].wait()
    a, b, h1, h2, hx, ys, zs, os = {}, {}, {}, {}, {}, {}, {}, {}
    a[0] = project(0)
    q1.wait_recv()
    sqp[c] += sqd[...]
    q2 = send(sqp.at[c, ox], sqx, s_q.at[1], r_q.at[1], x_peer)
    if chunks > 1:
        a[1] = project(1)
    for k in range(min(2, chunks)):
        b[k] = combine(k, a[k])
    q2.wait_recv()
    inv = lax.rsqrt((sqp[c, x] + sqx[...]) / width + EPS)
    loads[4].wait()
    loads[5].wait()
    for t in range(chunks + 3):
        if t + 2 < chunks:
            a[t + 2] = project(t + 2)
        if t < chunks:
            hx[t], h1[t] = activate(t, b[t], inv)
        if t + 2 < chunks:
            b[t + 2] = combine(t + 2, a[t + 2])
        if 0 <= t - 1 < chunks:
            if t == 1:
                loads[6].wait()
            h2[t - 1] = forward(t - 1, hx[t - 1])
            ys[t - 1] = lower(t - 1, h1[t - 1], h2[t - 1])
        if 0 <= t - 2 < chunks:
            zs[t - 2] = across(t - 2, ys[t - 2])
        if 0 <= t - 3 < chunks:
            os[t - 3] = finish(t - 3, zs[t - 3])
    for k in range(chunks):
        for copy in os[k]:
            copy.wait_recv()
    osum = osq[0] + osq[1] + osq[2] + osq[3]
    inv_out = lax.rsqrt(osum.reshape(own, LANES) / width + EPS)[:, :1]
    out_ref[...] = (mixed[...] * inv_out * og[...].astype(jnp.float32)).astype(out_ref.dtype)
    for copy in sends:
        copy.wait_send()


def fused_body(n_ra, width, tokens, norm_gain, w_gate, w_up, w_down, out_gain):
    count, depth = tokens.shape
    units = w_down.shape[0]
    own = count // n_ra
    rows, sub, quarter = count // CHUNKS, own // CHUNKS, count // CHUNKS // 4
    nz = n_ra // 2
    f32, bf16 = jnp.float32, jnp.bfloat16
    dma = pltpu.SemaphoreType.DMA
    per = [dma((CHUNKS,)) for _ in range(12)]
    return pl.pallas_call(
        functools.partial(kernel, n_ra, width),
        out_shape=jax.ShapeDtypeStruct((own, depth), bf16),
        in_specs=[pl.BlockSpec(memory_space=pl.ANY)] * 6,
        out_specs=pl.BlockSpec(memory_space=pltpu.VMEM),
        scratch_shapes=[
            pltpu.VMEM((count, depth), bf16),
            pltpu.VMEM((own, depth), bf16),
            pltpu.VMEM((1, depth), bf16),
            pltpu.VMEM((1, depth), bf16),
            pltpu.VMEM((depth, 2 * units), bf16),
            pltpu.VMEM((units, depth), bf16),
            pltpu.VMEM((CHUNKS, rows, depth), f32),
            pltpu.VMEM((CHUNKS, rows, depth), bf16),
            pltpu.VMEM((own, depth), f32),
            pltpu.VMEM((CHUNKS, 2, 2, quarter, 2 * units), f32),
            pltpu.VMEM((CHUNKS, 2, quarter, 2 * units), f32),
            pltpu.VMEM((CHUNKS, quarter, 2 * units), f32),
            pltpu.VMEM((2, 2, quarter, LANES), f32),
            pltpu.VMEM((2, quarter, LANES), f32),
            pltpu.VMEM((quarter, LANES), f32),
            pltpu.VMEM((CHUNKS, 2, 2, quarter, units), f32),
            pltpu.VMEM((CHUNKS, 2, nz, sub, depth), f32),
            pltpu.VMEM((CHUNKS, nz, sub, depth), f32),
            pltpu.VMEM((CHUNKS, nz - 1, sub, depth), f32),
            pltpu.VMEM((4, CHUNKS, sub, LANES), f32),
            dma((7,)),
            *per,
            dma((CHUNKS, nz - 1)),
            dma((CHUNKS, nz - 1)),
            dma((CHUNKS, 3)),
            dma((CHUNKS, 3)),
            dma((2,)),
            dma((2,)),
        ],
        compiler_params=pltpu.CompilerParams(
            collective_id=0, has_side_effects=True, vmem_limit_bytes=VMEM_BYTES),
    )(tokens, norm_gain.reshape(1, depth), w_gate, w_up, w_down, out_gain.reshape(1, depth))


def solution(mesh):
    n_ra, n_cb = mesh.shape["ra"], mesh.shape["cb"]

    def body(*args):
        tokens, w_down = args[0], args[4]
        count, depth = tokens.shape
        units = w_down.shape[0]
        width = depth * n_cb
        tiled = (
            n_cb == 4 and n_ra % 2 == 0 and n_ra > 2
            and count % (n_ra * CHUNKS * 8) == 0 and units % LANES == 0 and depth % TILE == 0
            and (count // CHUNKS // 4) % (count // n_ra // CHUNKS) == 0)
        if tiled:
            return fused_body(n_ra, width, *args)
        return plain_body(width, *args)

    return jax.shard_map(
        body,
        mesh=mesh,
        in_specs=(P(None, "cb"), P("cb"), P("cb", "ra"), P("cb", "ra"), P("ra", "cb"), P("cb")),
        out_specs=P("ra", "cb"),
        check_vma=False,
    )
```

```python
import functools

import jax
import jax.numpy as jnp
from jax import lax
from jax.experimental import pallas as pl
from jax.experimental.pallas import tpu as pltpu
from jax.sharding import PartitionSpec as P

EPS = 1e-06
LANES = 128
TILE = 256
PIECES = 3
SHARES = (1, 2, 2, 1, 1, 1)
UNITS = sum(SHARES)
VMEM_BYTES = 64 * 1024 * 1024 - 64 * 1024


def plain_body(width, tokens, norm_gain, w_gate, w_up, w_down, out_gain):
    xfloat = tokens.astype(jnp.float32)
    local_sq = jnp.sum(xfloat * xfloat, axis=1)
    scaled = (xfloat * norm_gain.astype(jnp.float32)).astype(jnp.bfloat16)
    gate_part = jnp.dot(scaled, w_gate, preferred_element_type=jnp.float32)
    up_part = jnp.dot(scaled, w_up, preferred_element_type=jnp.float32)
    total_sq, gate_sum, up_sum = lax.psum((local_sq, gate_part, up_part), "cb")
    inv_in = lax.rsqrt(total_sq / width + EPS)[:, None]
    hidden = (jax.nn.silu(gate_sum * inv_in) * (up_sum * inv_in)).astype(jnp.bfloat16)
    partial_down = jnp.dot(hidden, w_down, preferred_element_type=jnp.float32)
    own_rows = tokens.shape[0] // lax.axis_size("ra")
    first_row = lax.axis_index("ra") * own_rows
    down = lax.psum_scatter(partial_down, "ra", scatter_dimension=0, tiled=True)
    residual = lax.dynamic_slice_in_dim(xfloat, first_row, own_rows, 0)
    mixed = 0.1 * residual + down
    out_sq = lax.psum(jnp.sum(mixed * mixed, axis=1), "cb")
    inv_out = lax.rsqrt(out_sq / width + EPS)[:, None]
    return (mixed * inv_out * out_gain.astype(jnp.float32)).astype(jnp.bfloat16)


def kernel(n_ra, width, subs, *refs):
    it = iter(refs)

    def take(count):
        return [next(it) for _ in range(count)]

    n = len(subs)
    tok_hbm, ng_hbm, wg_hbm, wu_hbm, wd_hbm, og_hbm, out_ref = take(7)
    tok, rest, ng, og, wgu, wd, xs, mixed, sqp, sqd, sqx, osq = take(12)
    xb, part, prec, xrec, hid, dn, yrec, zrec = [take(n) for _ in range(8)]
    ld, lw, s_d, r_d, s_x, r_x, s_h, r_h, s_y, r_y, s_z, r_z, s_o, r_o, s_q, r_q = take(16)
    depth, units = xs.shape[1], wd.shape[0]
    own = rest.shape[0]
    base = [sum(subs[:k]) for k in range(n)]
    nz = n_ra // 2
    ra, cb = lax.axis_index("ra"), lax.axis_index("cb")
    c, x = lax.rem(cb, 2), lax.div(cb, 2)
    y, z = lax.rem(ra, 2), lax.div(ra, 2)
    oc, ox, oy = 1 - c, 1 - x, 1 - y
    core_peer = (ra, x * 2 + oc)
    x_peer = (ra, ox * 2 + c)
    diag_peer = (ra, ox * 2 + oc)
    y_peer = (z * 2 + oy, cb)
    z_peers = [(lax.rem(z + d, nz) * 2 + y, cb) for d in range(1, nz)]
    mesh_id = pl.DeviceIdType.MESH
    pieces = column_pieces(2 * units)
    halves = [(0, depth // 2), (depth // 2, depth // 2)]

    early = [
        pltpu.make_async_copy(tok_hbm, tok, ld.at[0]),
        pltpu.make_async_copy(ng_hbm, ng, ld.at[1]),
    ]
    weights = []
    for p, (start, size) in enumerate(pieces):
        got = []
        for i, (ref, low) in enumerate(((wg_hbm, 0), (wu_hbm, units))):
            lo, hi = max(start, low), min(start + size, low + units)
            if lo < hi:
                got.append(pltpu.make_async_copy(
                    ref.at[:, pl.ds(lo - low, hi - lo)], wgu.at[:, pl.ds(lo, hi - lo)], lw.at[p, i]))
        weights.append(got)
    late = [
        pltpu.make_async_copy(tok_hbm.at[pl.ds(pl.multiple_of(ra * own, own), own)], rest, ld.at[2]),
        pltpu.make_async_copy(og_hbm, og, ld.at[3]),
        pltpu.make_async_copy(wd_hbm, wd, ld.at[4]),
    ]
    for load in early + sum(weights, []) + late:
        load.start()

    barrier = pltpu.get_barrier_semaphore()
    peers = [core_peer, x_peer, diag_peer, y_peer] + z_peers
    for peer in peers:
        pl.semaphore_signal(barrier, inc=1, device_id=peer, device_id_type=mesh_id)

    sends = []

    def send(src, dst, s, r, peer):
        copy = pltpu.make_async_remote_copy(
            src_ref=src, dst_ref=dst, send_sem=s, recv_sem=r,
            device_id=peer, device_id_type=mesh_id)
        copy.start()
        sends.append(copy)
        return copy

    def project(k, p):
        with jax.named_scope(f"project{k}"):
            start, size = pieces[p]
            cols = pl.ds(start, size)
            got = jnp.dot(xb[k][...], wgu[:, cols], preferred_element_type=jnp.float32)
            part[k][:, :, :, cols] = got.reshape(2, 2, part[k].shape[2], size)

    def to_core(k, cols, p):
        return send(part[k].at[oc, :, :, cols], prec[k].at[:, :, cols], s_d.at[k, p], r_d.at[k, p], core_peer)

    def combine(k, copy, start, size, p):
        with jax.named_scope(f"combine{k}"):
            copy.wait_recv()
            cols = pl.ds(start, size)
            part[k][c, :, :, cols] += prec[k][:, :, cols]
            return send(part[k].at[c, ox, :, cols], xrec[k].at[:, cols], s_x.at[k, p], r_x.at[k, p], x_peer)

    def whole(k):
        for p in range(len(pieces)):
            project(k, p)
        return to_core(k, pl.ds(0, 2 * units), 0)

    def join(k, copy):
        return [combine(k, copy, 0, 2 * units, 0)]

    def activate(k, copies, inv):
        with jax.named_scope(f"activate{k}"):
            for copy in copies:
                copy.wait_recv()
            scale = inv[:part[k].shape[2], k:k + 1]
            gate = (part[k][c, x, :, :units] + xrec[k][:, :units]) * scale
            up = (part[k][c, x, :, units:] + xrec[k][:, units:]) * scale
            val = gate / (1.0 + jnp.exp(-gate)) * up
            hid[k][c, x] = val.astype(jnp.bfloat16).astype(jnp.float32)
            block = hid[k].at[c, x]
            hx = send(block, block, s_h.at[k, 0], r_h.at[k, 0], x_peer)
            h1 = send(block, block, s_h.at[k, 1], r_h.at[k, 1], core_peer)
            return hx, h1

    def forward(k, hx):
        with jax.named_scope(f"forward{k}"):
            hx.wait_recv()
            block = hid[k].at[c, ox]
            return send(block, block, s_h.at[k, 2], r_h.at[k, 2], core_peer)

    def lower(k, h1, h2):
        with jax.named_scope(f"lower{k}"):
            h1.wait_recv()
            h2.wait_recv()
            hb = hid[k][...].reshape(n_ra * subs[k], units).astype(jnp.bfloat16)
            out = []
            for h, (start, size) in enumerate(halves):
                cols = pl.ds(start, size)
                got = jnp.dot(hb, wd[:, cols], preferred_element_type=jnp.float32)
                dn[k][:, :, :, cols] = got.reshape(2, nz, subs[k], size)
                out.append(send(dn[k].at[oy, :, :, cols], yrec[k].at[:, :, cols],
                                s_y.at[k, h], r_y.at[k, h], y_peer))
            return out

    def across(k, copies):
        with jax.named_scope(f"across{k}"):
            out = []
            for h, (start, size) in enumerate(halves):
                cols = pl.ds(start, size)
                copies[h].wait_recv()
                dn[k][y, :, :, cols] += yrec[k][:, :, cols]
                for d in range(1, nz):
                    out.append(send(
                        dn[k].at[y, lax.rem(z + d, nz), :, cols], zrec[k].at[d - 1, :, cols],
                        s_z.at[k, h, d - 1], r_z.at[k, h, d - 1], z_peers[d - 1]))
            return out

    def finish(k, copies):
        with jax.named_scope(f"finish{k}"):
            for copy in copies:
                copy.wait_recv()
            got = dn[k][y, z]
            for d in range(nz - 1):
                got = got + zrec[k][d]
            at = pl.ds(base[k], subs[k])
            got = mixed[at, :] + got
            mixed[at, :] = got
            osq[0, at, :] = jnp.broadcast_to(jnp.sum(got * got, axis=1, keepdims=True), (subs[k], LANES))
            return [
                send(osq.at[0, at], osq.at[i + 1, at], s_o.at[k, i], r_o.at[k, i], peer)
                for i, peer in enumerate((core_peer, x_peer, diag_peer))]

    def fill(k):
        xb[k][...] = jnp.concatenate(
            [xs[pl.ds((zz * 2 + yy) * own + base[k], subs[k]), :] for yy in range(2) for zz in range(nz)],
            axis=0).astype(jnp.bfloat16)

    with jax.named_scope("tokens"):
        for load in early:
            load.wait()
    with jax.named_scope("scale"):
        gain = ng[...].astype(jnp.float32)
        for d in range(n_ra):
            at = pl.ds(d * own, own)
            xs[at, :] = tok[at, :].astype(jnp.float32) * gain
        fill(0)
    with jax.named_scope("enter"):
        pl.semaphore_wait(barrier, len(peers))

    a, b, h1, h2, hx, ys, zs, os = {}, {}, {}, {}, {}, {}, {}, {}
    heads, b[0] = [], []
    for p, (start, size) in enumerate(pieces):
        with jax.named_scope("weights"):
            for load in weights[p]:
                load.wait()
        project(0, p)
        heads.append(to_core(0, pl.ds(start, size), p))
        if p > 0:
            b[0].append(combine(0, heads[p - 1], *pieces[p - 1], p - 1))
    with jax.named_scope("squares"):
        lane = lax.broadcasted_iota(jnp.int32, (own, LANES), 1)
        sqp[...] = jnp.zeros_like(sqp)
        for d in range(n_ra):
            xf = tok[pl.ds(d * own, own), :].astype(jnp.float32)
            sq = jnp.broadcast_to(jnp.sum(xf * xf, axis=1, keepdims=True), (own, LANES))
            for k in range(n):
                at = ((d % 2) * nz + d // 2) * subs[k]
                quarter = nz * subs[k] // 2
                q, off = at // quarter, at % quarter
                val = jnp.where(lane[:subs[k]] == k, sq[base[k]:base[k] + subs[k]], 0.0)
                sqp[q // 2, q % 2, pl.ds(off, subs[k]), :] += val
        q1 = send(sqp.at[oc], sqd, s_q.at[0], r_q.at[0], core_peer)
    last = len(pieces) - 1
    b[0].append(combine(0, heads[last], *pieces[last], last))
    fill(1)
    a[1] = whole(1)
    q1.wait_recv()
    sqp[c] += sqd[...]
    q2 = send(sqp.at[c, ox], sqx, s_q.at[1], r_q.at[1], x_peer)
    b[1] = join(1, a[1])
    for k in range(2, n):
        fill(k)
    for load in late:
        load.wait()
    mixed[...] = 0.1 * rest[...].astype(jnp.float32)
    for t in range(n + 3):
        if t + 2 < n:
            a[t + 2] = whole(t + 2)
        if t == 0:
            q2.wait_recv()
            inv = lax.rsqrt((sqp[c, x] + sqx[...]) / width + EPS)
        if t < n:
            hx[t], h1[t] = activate(t, b[t], inv)
        if t + 2 < n:
            b[t + 2] = join(t + 2, a[t + 2])
        if 0 <= t - 1 < n:
            h2[t - 1] = forward(t - 1, hx[t - 1])
            ys[t - 1] = lower(t - 1, h1[t - 1], h2[t - 1])
        if 0 <= t - 2 < n:
            zs[t - 2] = across(t - 2, ys[t - 2])
        if 0 <= t - 3 < n:
            os[t - 3] = finish(t - 3, zs[t - 3])
    with jax.named_scope("norm"):
        for k in range(n):
            for copy in os[k]:
                copy.wait_recv()
        osum = osq[0] + osq[1] + osq[2] + osq[3]
        inv_out = lax.rsqrt(osum / width + EPS)[:, :1]
        out_ref[...] = (mixed[...] * inv_out * og[...].astype(jnp.float32)).astype(out_ref.dtype)
    with jax.named_scope("drain"):
        for copy in sends:
            copy.wait_send()


def column_pieces(total):
    tiles = total // TILE
    cuts = [tiles * i // PIECES * TILE for i in range(PIECES)] + [total]
    return [(lo, hi - lo) for lo, hi in zip(cuts[:-1], cuts[1:])]


def chunk_rows(own):
    unit = own // UNITS
    return [unit * share for share in SHARES]


def fused_body(n_ra, width, tokens, norm_gain, w_gate, w_up, w_down, out_gain):
    count, depth = tokens.shape
    units = w_down.shape[0]
    own = count // n_ra
    subs = chunk_rows(own)
    n, nz = len(subs), n_ra // 2
    f32, bf16 = jnp.float32, jnp.bfloat16
    dma = pltpu.SemaphoreType.DMA
    quarters = [n_ra * sub // 4 for sub in subs]
    most = max(quarters)
    return pl.pallas_call(
        functools.partial(kernel, n_ra, width, subs),
        out_shape=jax.ShapeDtypeStruct((own, depth), bf16),
        in_specs=[pl.BlockSpec(memory_space=pl.ANY)] * 6,
        out_specs=pl.BlockSpec(memory_space=pltpu.VMEM),
        scratch_shapes=[
            pltpu.VMEM((count, depth), bf16),
            pltpu.VMEM((own, depth), bf16),
            pltpu.VMEM((1, depth), bf16),
            pltpu.VMEM((1, depth), bf16),
            pltpu.VMEM((depth, 2 * units), bf16),
            pltpu.VMEM((units, depth), bf16),
            pltpu.VMEM((count, depth), f32),
            pltpu.VMEM((own, depth), f32),
            pltpu.VMEM((2, 2, most, LANES), f32),
            pltpu.VMEM((2, most, LANES), f32),
            pltpu.VMEM((most, LANES), f32),
            pltpu.VMEM((4, own, LANES), f32),
            *[pltpu.VMEM((n_ra * sub, depth), bf16) for sub in subs],
            *[pltpu.VMEM((2, 2, quarter, 2 * units), f32) for quarter in quarters],
            *[pltpu.VMEM((2, quarter, 2 * units), f32) for quarter in quarters],
            *[pltpu.VMEM((quarter, 2 * units), f32) for quarter in quarters],
            *[pltpu.VMEM((2, 2, quarter, units), f32) for quarter in quarters],
            *[pltpu.VMEM((2, nz, sub, depth), f32) for sub in subs],
            *[pltpu.VMEM((nz, sub, depth), f32) for sub in subs],
            *[pltpu.VMEM((nz - 1, sub, depth), f32) for sub in subs],
            dma((5,)),
            dma((PIECES, 2)),
            *[dma((n, PIECES)) for _ in range(4)],
            *[dma((n, 3)) for _ in range(2)],
            *[dma((n, 2)) for _ in range(2)],
            *[dma((n, 2, nz - 1)) for _ in range(2)],
            *[dma((n, 3)) for _ in range(2)],
            *[dma((2,)) for _ in range(2)],
        ],
        compiler_params=pltpu.CompilerParams(
            collective_id=0, has_side_effects=True, vmem_limit_bytes=VMEM_BYTES),
    )(tokens, norm_gain.reshape(1, depth), w_gate, w_up, w_down, out_gain.reshape(1, depth))


def solution(mesh):
    n_ra, n_cb = mesh.shape["ra"], mesh.shape["cb"]

    def body(*args):
        tokens, w_down = args[0], args[4]
        count, depth = tokens.shape
        units = w_down.shape[0]
        width = depth * n_cb
        tiled = (
            n_cb == 4 and n_ra % 4 == 0 and n_ra > 2
            and count % (n_ra * UNITS * 8) == 0 and units % LANES == 0 and depth % TILE == 0)
        if tiled:
            return fused_body(n_ra, width, *args)
        return plain_body(width, *args)

    return jax.shard_map(
        body,
        mesh=mesh,
        in_specs=(P(None, "cb"), P("cb"), P("cb", "ra"), P("cb", "ra"), P("ra", "cb"), P("cb")),
        out_specs=P("ra", "cb"),
        check_vma=False,
    )
```

```python
import functools

import jax
import jax.numpy as jnp
from jax import lax
from jax.experimental import pallas as pl
from jax.experimental.pallas import tpu as pltpu
from jax.sharding import PartitionSpec as P

EPS = 1e-06
LANES = 128
TILE = 256
PIECES = 3
SLICES = 2
SHARES = (1, 2, 2, 1, 1, 1)
UNITS = sum(SHARES)
VMEM_BYTES = 64 * 1024 * 1024 - 64 * 1024


def plain_body(width, tokens, norm_gain, w_gate, w_up, w_down, out_gain):
    xfloat = tokens.astype(jnp.float32)
    local_sq = jnp.sum(xfloat * xfloat, axis=1)
    scaled = (xfloat * norm_gain.astype(jnp.float32)).astype(jnp.bfloat16)
    gate_part = jnp.dot(scaled, w_gate, preferred_element_type=jnp.float32)
    up_part = jnp.dot(scaled, w_up, preferred_element_type=jnp.float32)
    total_sq, gate_sum, up_sum = lax.psum((local_sq, gate_part, up_part), "cb")
    inv_in = lax.rsqrt(total_sq / width + EPS)[:, None]
    hidden = (jax.nn.silu(gate_sum * inv_in) * (up_sum * inv_in)).astype(jnp.bfloat16)
    partial_down = jnp.dot(hidden, w_down, preferred_element_type=jnp.float32)
    own_rows = tokens.shape[0] // lax.axis_size("ra")
    first_row = lax.axis_index("ra") * own_rows
    down = lax.psum_scatter(partial_down, "ra", scatter_dimension=0, tiled=True)
    residual = lax.dynamic_slice_in_dim(xfloat, first_row, own_rows, 0)
    mixed = 0.1 * residual + down
    out_sq = lax.psum(jnp.sum(mixed * mixed, axis=1), "cb")
    inv_out = lax.rsqrt(out_sq / width + EPS)[:, None]
    return (mixed * inv_out * out_gain.astype(jnp.float32)).astype(jnp.bfloat16)


def kernel(n_ra, width, subs, *refs):
    it = iter(refs)

    def take(count):
        return [next(it) for _ in range(count)]

    n = len(subs)
    tok_hbm, ng_hbm, wg_hbm, wu_hbm, wd_hbm, og_hbm, out_ref = take(7)
    tok, rest, ng, og, wgu, wd, xs, mixed, sqp, sqd, sqx, osq = take(12)
    xb, part, prec, xrec, hid, dn, yrec, zrec = [take(n) for _ in range(8)]
    ld, lw, s_d, r_d, s_x, r_x, s_h, r_h, s_y, r_y, s_z, r_z, s_o, r_o, s_q, r_q = take(16)
    depth, units = xs.shape[1], wd.shape[0]
    own = rest.shape[0]
    base = [sum(subs[:k]) for k in range(n)]
    nz = n_ra // 2
    ra, cb = lax.axis_index("ra"), lax.axis_index("cb")
    c, x = lax.rem(cb, 2), lax.div(cb, 2)
    y, z = lax.rem(ra, 2), lax.div(ra, 2)
    oc, ox, oy = 1 - c, 1 - x, 1 - y
    core_peer = (ra, x * 2 + oc)
    x_peer = (ra, ox * 2 + c)
    diag_peer = (ra, ox * 2 + oc)
    y_peer = (z * 2 + oy, cb)
    z_peers = [(lax.rem(z + d, nz) * 2 + y, cb) for d in range(1, nz)]
    mesh_id = pl.DeviceIdType.MESH
    pieces = column_pieces(2 * units)
    slices = [(i * depth // SLICES, depth // SLICES) for i in range(SLICES)]

    early = [
        pltpu.make_async_copy(tok_hbm, tok, ld.at[0]),
        pltpu.make_async_copy(ng_hbm, ng, ld.at[1]),
    ]
    weights = []
    for p, (start, size) in enumerate(pieces):
        got = []
        for i, (ref, low) in enumerate(((wg_hbm, 0), (wu_hbm, units))):
            lo, hi = max(start, low), min(start + size, low + units)
            if lo < hi:
                got.append(pltpu.make_async_copy(
                    ref.at[:, pl.ds(lo - low, hi - lo)], wgu.at[:, pl.ds(lo, hi - lo)], lw.at[p, i]))
        weights.append(got)
    late = [
        pltpu.make_async_copy(tok_hbm.at[pl.ds(pl.multiple_of(ra * own, own), own)], rest, ld.at[2]),
        pltpu.make_async_copy(og_hbm, og, ld.at[3]),
        pltpu.make_async_copy(wd_hbm, wd, ld.at[4]),
    ]
    for load in early + sum(weights, []) + late:
        load.start()

    barrier = pltpu.get_barrier_semaphore()
    peers = [core_peer, x_peer, diag_peer, y_peer] + z_peers
    for peer in peers:
        pl.semaphore_signal(barrier, inc=1, device_id=peer, device_id_type=mesh_id)

    sends = []

    def send(src, dst, s, r, peer):
        copy = pltpu.make_async_remote_copy(
            src_ref=src, dst_ref=dst, send_sem=s, recv_sem=r,
            device_id=peer, device_id_type=mesh_id)
        copy.start()
        sends.append(copy)
        return copy

    def project(k, p):
        with jax.named_scope(f"project{k}"):
            start, size = pieces[p]
            cols = pl.ds(start, size)
            got = jnp.dot(xb[k][...], wgu[:, cols], preferred_element_type=jnp.float32)
            part[k][:, :, :, cols] = got.reshape(2, 2, part[k].shape[2], size)

    def to_core(k, cols, p):
        return send(part[k].at[oc, :, :, cols], prec[k].at[:, :, cols], s_d.at[k, p], r_d.at[k, p], core_peer)

    def combine(k, copy, start, size, p):
        with jax.named_scope(f"combine{k}"):
            copy.wait_recv()
            cols = pl.ds(start, size)
            part[k][c, :, :, cols] += prec[k][:, :, cols]
            return send(part[k].at[c, ox, :, cols], xrec[k].at[:, cols], s_x.at[k, p], r_x.at[k, p], x_peer)

    def whole(k):
        for p in range(len(pieces)):
            project(k, p)
        return to_core(k, pl.ds(0, 2 * units), 0)

    def join(k, copy):
        return [combine(k, copy, 0, 2 * units, 0)]

    def activate(k, copies, inv):
        with jax.named_scope(f"activate{k}"):
            for copy in copies:
                copy.wait_recv()
            scale = inv[:part[k].shape[2], k:k + 1]
            gate = (part[k][c, x, :, :units] + xrec[k][:, :units]) * scale
            up = (part[k][c, x, :, units:] + xrec[k][:, units:]) * scale
            val = gate / (1.0 + jnp.exp(-gate)) * up
            hid[k][c, x] = val.astype(jnp.bfloat16).astype(jnp.float32)
            block = hid[k].at[c, x]
            hx = send(block, block, s_h.at[k, 0], r_h.at[k, 0], x_peer)
            h1 = send(block, block, s_h.at[k, 1], r_h.at[k, 1], core_peer)
            return hx, h1

    def forward(k, hx):
        with jax.named_scope(f"forward{k}"):
            hx.wait_recv()
            block = hid[k].at[c, ox]
            return send(block, block, s_h.at[k, 2], r_h.at[k, 2], core_peer)

    def lower(k, h1, h2):
        with jax.named_scope(f"lower{k}"):
            h1.wait_recv()
            h2.wait_recv()
            hb = hid[k][...].reshape(n_ra * subs[k], units).astype(jnp.bfloat16)
            out = []
            for h, (start, size) in enumerate(slices):
                cols = pl.ds(start, size)
                got = jnp.dot(hb, wd[:, cols], preferred_element_type=jnp.float32)
                dn[k][:, :, :, cols] = got.reshape(2, nz, subs[k], size)
                out.append(send(dn[k].at[oy, :, :, cols], yrec[k].at[:, :, cols],
                                s_y.at[k, h], r_y.at[k, h], y_peer))
            return out

    def across(k, copies):
        with jax.named_scope(f"across{k}"):
            out = []
            for h, (start, size) in enumerate(slices):
                cols = pl.ds(start, size)
                copies[h].wait_recv()
                dn[k][y, :, :, cols] += yrec[k][:, :, cols]
                for d in range(1, nz):
                    out.append(send(
                        dn[k].at[y, lax.rem(z + d, nz), :, cols], zrec[k].at[d - 1, :, cols],
                        s_z.at[k, h, d - 1], r_z.at[k, h, d - 1], z_peers[d - 1]))
            return out

    def finish(k, copies):
        with jax.named_scope(f"finish{k}"):
            for copy in copies:
                copy.wait_recv()
            got = dn[k][y, z]
            for d in range(nz - 1):
                got = got + zrec[k][d]
            at = pl.ds(base[k], subs[k])
            got = mixed[at, :] + got
            mixed[at, :] = got
            osq[0, at, :] = jnp.broadcast_to(jnp.sum(got * got, axis=1, keepdims=True), (subs[k], LANES))
            return [
                send(osq.at[0, at], osq.at[i + 1, at], s_o.at[k, i], r_o.at[k, i], peer)
                for i, peer in enumerate((core_peer, x_peer, diag_peer))]

    def fill(k):
        xb[k][...] = jnp.concatenate(
            [xs[pl.ds((zz * 2 + yy) * own + base[k], subs[k]), :] for yy in range(2) for zz in range(nz)],
            axis=0).astype(jnp.bfloat16)

    def squares():
        with jax.named_scope("squares"):
            lane = lax.broadcasted_iota(jnp.int32, (own, LANES), 1)
            sqp[...] = jnp.zeros_like(sqp)
            for d in range(n_ra):
                xf = tok[pl.ds(d * own, own), :].astype(jnp.float32)
                sq = jnp.broadcast_to(jnp.sum(xf * xf, axis=1, keepdims=True), (own, LANES))
                for k in range(n):
                    at = ((d % 2) * nz + d // 2) * subs[k]
                    quarter = nz * subs[k] // 2
                    q, off = at // quarter, at % quarter
                    val = jnp.where(lane[:subs[k]] == k, sq[base[k]:base[k] + subs[k]], 0.0)
                    sqp[q // 2, q % 2, pl.ds(off, subs[k]), :] += val
            return send(sqp.at[oc], sqd, s_q.at[0], r_q.at[0], core_peer)

    with jax.named_scope("tokens"):
        for load in early:
            load.wait()
    with jax.named_scope("scale"):
        gain = ng[...].astype(jnp.float32).reshape(1, depth)
        for d in range(n_ra):
            at = pl.ds(d * own, own)
            xs[at, :] = tok[at, :].astype(jnp.float32) * gain
        fill(0)
    with jax.named_scope("enter"):
        pl.semaphore_wait(barrier, len(peers))

    a, b, h1, h2, hx, ys, zs, os = {}, {}, {}, {}, {}, {}, {}, {}
    b[0], b[1], waiting = [], [], []
    for k in range(2):
        for p, (start, size) in enumerate(pieces):
            if k == 0:
                with jax.named_scope("weights"):
                    for load in weights[p]:
                        load.wait()
            project(k, p)
            waiting.append((k, p, to_core(k, pl.ds(start, size), p)))
            if k == 0 and p == 0:
                q1 = squares()
            if len(waiting) > 1:
                kk, pp, copy = waiting.pop(0)
                b[kk].append(combine(kk, copy, *pieces[pp], pp))
            if k == 0 and p == 1:
                with jax.named_scope("share"):
                    q1.wait_recv()
                    sqp[c] += sqd[...]
                    q2 = send(sqp.at[c, ox], sqx, s_q.at[1], r_q.at[1], x_peer)
                fill(1)
    for kk, pp, copy in waiting:
        b[kk].append(combine(kk, copy, *pieces[pp], pp))
    for k in range(2, n):
        fill(k)
    for load in late:
        load.wait()
    mixed[...] = 0.1 * rest[...].astype(jnp.float32)
    for t in range(n + 3):
        if t + 2 < n:
            a[t + 2] = whole(t + 2)
        if t == 0:
            q2.wait_recv()
            inv = lax.rsqrt((sqp[c, x] + sqx[...]) / width + EPS)
        if t < n:
            hx[t], h1[t] = activate(t, b[t], inv)
        if t + 2 < n:
            b[t + 2] = join(t + 2, a[t + 2])
        if 0 <= t - 1 < n:
            h2[t - 1] = forward(t - 1, hx[t - 1])
        if t == n and n > 2:
            zs[n - 3] = across(n - 3, ys[n - 3])
        if 0 <= t - 1 < n:
            ys[t - 1] = lower(t - 1, h1[t - 1], h2[t - 1])
        if t == n and n > 3:
            os[n - 4] = finish(n - 4, zs[n - 4])
        if 0 <= t - 2 < n and t != n - 1:
            zs[t - 2] = across(t - 2, ys[t - 2])
        if 0 <= t - 3 < n and t != n - 1:
            os[t - 3] = finish(t - 3, zs[t - 3])
    with jax.named_scope("norm"):
        for k in range(n):
            for copy in os[k]:
                copy.wait_recv()
        osum = osq[0] + osq[1] + osq[2] + osq[3]
        inv_out = lax.rsqrt(osum / width + EPS)[:, :1]
        out_ref[...] = (mixed[...] * inv_out * og[...].astype(jnp.float32).reshape(1, depth)).astype(out_ref.dtype)
    with jax.named_scope("drain"):
        for copy in sends:
            copy.wait_send()


def column_pieces(total):
    tiles = total // TILE
    cuts = [tiles * i // PIECES * TILE for i in range(PIECES)] + [total]
    return [(lo, hi - lo) for lo, hi in zip(cuts[:-1], cuts[1:])]


def chunk_rows(own):
    unit = own // UNITS
    return [unit * share for share in SHARES]


def fused_body(n_ra, width, tokens, norm_gain, w_gate, w_up, w_down, out_gain):
    count, depth = tokens.shape
    units = w_down.shape[0]
    own = count // n_ra
    subs = chunk_rows(own)
    n, nz = len(subs), n_ra // 2
    f32, bf16 = jnp.float32, jnp.bfloat16
    dma = pltpu.SemaphoreType.DMA
    quarters = [n_ra * sub // 4 for sub in subs]
    most = max(quarters)
    return pl.pallas_call(
        functools.partial(kernel, n_ra, width, subs),
        out_shape=jax.ShapeDtypeStruct((own, depth), bf16),
        in_specs=[pl.BlockSpec(memory_space=pl.ANY)] * 6,
        out_specs=pl.BlockSpec(memory_space=pltpu.VMEM),
        scratch_shapes=[
            pltpu.VMEM((count, depth), bf16),
            pltpu.VMEM((own, depth), bf16),
            pltpu.VMEM((depth,), bf16),
            pltpu.VMEM((depth,), bf16),
            pltpu.VMEM((depth, 2 * units), bf16),
            pltpu.VMEM((units, depth), bf16),
            pltpu.VMEM((count, depth), f32),
            pltpu.VMEM((own, depth), f32),
            pltpu.VMEM((2, 2, most, LANES), f32),
            pltpu.VMEM((2, most, LANES), f32),
            pltpu.VMEM((most, LANES), f32),
            pltpu.VMEM((4, own, LANES), f32),
            *[pltpu.VMEM((n_ra * sub, depth), bf16) for sub in subs],
            *[pltpu.VMEM((2, 2, quarter, 2 * units), f32) for quarter in quarters],
            *[pltpu.VMEM((2, quarter, 2 * units), f32) for quarter in quarters],
            *[pltpu.VMEM((quarter, 2 * units), f32) for quarter in quarters],
            *[pltpu.VMEM((2, 2, quarter, units), f32) for quarter in quarters],
            *[pltpu.VMEM((2, nz, sub, depth), f32) for sub in subs],
            *[pltpu.VMEM((nz, sub, depth), f32) for sub in subs],
            *[pltpu.VMEM((nz - 1, sub, depth), f32) for sub in subs],
            dma((5,)),
            dma((PIECES, 2)),
            *[dma((n, PIECES)) for _ in range(4)],
            *[dma((n, 3)) for _ in range(2)],
            *[dma((n, SLICES)) for _ in range(2)],
            *[dma((n, SLICES, nz - 1)) for _ in range(2)],
            *[dma((n, 3)) for _ in range(2)],
            *[dma((2,)) for _ in range(2)],
        ],
        compiler_params=pltpu.CompilerParams(
            collective_id=0, has_side_effects=True, vmem_limit_bytes=VMEM_BYTES),
    )(tokens, norm_gain, w_gate, w_up, w_down, out_gain)


def solution(mesh):
    n_ra, n_cb = mesh.shape["ra"], mesh.shape["cb"]

    def body(*args):
        tokens, w_down = args[0], args[4]
        count, depth = tokens.shape
        units = w_down.shape[0]
        width = depth * n_cb
        tiled = (
            n_cb == 4 and n_ra % 4 == 0 and n_ra > 2
            and count % (n_ra * UNITS * 8) == 0 and units % LANES == 0 and depth % TILE == 0
            and depth % (SLICES * LANES) == 0)
        if tiled:
            return fused_body(n_ra, width, *args)
        return plain_body(width, *args)

    return jax.shard_map(
        body,
        mesh=mesh,
        in_specs=(P(None, "cb"), P("cb"), P("cb", "ra"), P("cb", "ra"), P("ra", "cb"), P("cb")),
        out_specs=P("ra", "cb"),
        check_vma=False,
    )
```

```python
import functools

import jax
import jax.numpy as jnp
from jax import lax
from jax.experimental import pallas as pl
from jax.experimental.pallas import tpu as pltpu
from jax.sharding import PartitionSpec as P

EPS = 1e-06
LANES = 128
TILE = 256
PIECES = 3
SLICES = 2
SHARES = (1, 2, 2, 1, 1, 1)
UNITS = sum(SHARES)
VMEM_BYTES = 64 * 1024 * 1024 - 64 * 1024


def plain_body(width, tokens, norm_gain, w_gate, w_up, w_down, out_gain):
    xfloat = tokens.astype(jnp.float32)
    local_sq = jnp.sum(xfloat * xfloat, axis=1)
    scaled = (xfloat * norm_gain.astype(jnp.float32)).astype(jnp.bfloat16)
    gate_part = jnp.dot(scaled, w_gate, preferred_element_type=jnp.float32)
    up_part = jnp.dot(scaled, w_up, preferred_element_type=jnp.float32)
    total_sq, gate_sum, up_sum = lax.psum((local_sq, gate_part, up_part), "cb")
    inv_in = lax.rsqrt(total_sq / width + EPS)[:, None]
    hidden = (jax.nn.silu(gate_sum * inv_in) * (up_sum * inv_in)).astype(jnp.bfloat16)
    partial_down = jnp.dot(hidden, w_down, preferred_element_type=jnp.float32)
    own_rows = tokens.shape[0] // lax.axis_size("ra")
    first_row = lax.axis_index("ra") * own_rows
    down = lax.psum_scatter(partial_down, "ra", scatter_dimension=0, tiled=True)
    residual = lax.dynamic_slice_in_dim(xfloat, first_row, own_rows, 0)
    mixed = 0.1 * residual + down
    out_sq = lax.psum(jnp.sum(mixed * mixed, axis=1), "cb")
    inv_out = lax.rsqrt(out_sq / width + EPS)[:, None]
    return (mixed * inv_out * out_gain.astype(jnp.float32)).astype(jnp.bfloat16)


def kernel(n_ra, width, subs, *refs):
    it = iter(refs)

    def take(count):
        return [next(it) for _ in range(count)]

    n = len(subs)
    tok_hbm, ng_hbm, wg_hbm, wu_hbm, wd_hbm, og_hbm, out_ref = take(7)
    tok, rest, ng, og, wgu, wd, xs, mixed, sqp, sqd, sqx, osq = take(12)
    xb, part, prec, xrec, hid, dn, yrec, zrec = [take(n) for _ in range(8)]
    ld, lw, s_d, r_d, s_x, r_x, s_h, r_h, s_y, r_y, s_z, r_z, s_o, r_o, s_q, r_q = take(16)
    depth, units = xs.shape[1], wd.shape[0]
    own = rest.shape[0]
    base = [sum(subs[:k]) for k in range(n)]
    nz = n_ra // 2
    ra, cb = lax.axis_index("ra"), lax.axis_index("cb")
    c, x = lax.rem(cb, 2), lax.div(cb, 2)
    y, z = lax.rem(ra, 2), lax.div(ra, 2)
    oc, ox, oy = 1 - c, 1 - x, 1 - y
    core_peer = (ra, x * 2 + oc)
    x_peer = (ra, ox * 2 + c)
    diag_peer = (ra, ox * 2 + oc)
    y_peer = (z * 2 + oy, cb)
    z_peers = [(lax.rem(z + d, nz) * 2 + y, cb) for d in range(1, nz)]
    mesh_id = pl.DeviceIdType.MESH
    pieces = column_pieces(2 * units)
    slices = [(i * depth // SLICES, depth // SLICES) for i in range(SLICES)]

    early = [
        pltpu.make_async_copy(tok_hbm, tok, ld.at[0]),
        pltpu.make_async_copy(ng_hbm, ng, ld.at[1]),
    ]
    weights = []
    for p, (start, size) in enumerate(pieces):
        got = []
        for i, (ref, low) in enumerate(((wg_hbm, 0), (wu_hbm, units))):
            lo, hi = max(start, low), min(start + size, low + units)
            if lo < hi:
                got.append(pltpu.make_async_copy(
                    ref.at[:, pl.ds(lo - low, hi - lo)], wgu.at[:, pl.ds(lo, hi - lo)], lw.at[p, i]))
        weights.append(got)
    late = [
        pltpu.make_async_copy(tok_hbm.at[pl.ds(pl.multiple_of(ra * own, own), own)], rest, ld.at[2]),
        pltpu.make_async_copy(og_hbm, og, ld.at[3]),
        pltpu.make_async_copy(wd_hbm, wd, ld.at[4]),
    ]
    for load in early + sum(weights, []) + late:
        load.start()

    barrier = pltpu.get_barrier_semaphore()
    peers = [core_peer, x_peer, diag_peer, y_peer] + z_peers
    for peer in peers:
        pl.semaphore_signal(barrier, inc=1, device_id=peer, device_id_type=mesh_id)

    sends = []

    def send(src, dst, s, r, peer):
        copy = pltpu.make_async_remote_copy(
            src_ref=src, dst_ref=dst, send_sem=s, recv_sem=r,
            device_id=peer, device_id_type=mesh_id)
        copy.start()
        sends.append(copy)
        return copy

    def project(k, p):
        with jax.named_scope(f"project{k}"):
            start, size = pieces[p]
            cols = pl.ds(start, size)
            got = jnp.dot(xb[k][...], wgu[:, cols], preferred_element_type=jnp.float32)
            part[k][:, :, :, cols] = got.reshape(2, 2, part[k].shape[2], size)

    def to_core(k, cols, p):
        return send(part[k].at[oc, :, :, cols], prec[k].at[:, :, cols], s_d.at[k, p], r_d.at[k, p], core_peer)

    def combine(k, copy, start, size, p):
        with jax.named_scope(f"combine{k}"):
            copy.wait_recv()
            cols = pl.ds(start, size)
            part[k][c, :, :, cols] += prec[k][:, :, cols]
            return send(part[k].at[c, ox, :, cols], xrec[k].at[:, cols], s_x.at[k, p], r_x.at[k, p], x_peer)

    def whole(k):
        for p in range(len(pieces)):
            project(k, p)
        return to_core(k, pl.ds(0, 2 * units), 0)

    def join(k, copy):
        return [combine(k, copy, 0, 2 * units, 0)]

    def activate(k, copies, inv):
        with jax.named_scope(f"activate{k}"):
            for copy in copies:
                copy.wait_recv()
            scale = inv[:part[k].shape[2], k:k + 1]
            gate = (part[k][c, x, :, :units] + xrec[k][:, :units]) * scale
            up = (part[k][c, x, :, units:] + xrec[k][:, units:]) * scale
            val = gate / (1.0 + jnp.exp(-gate)) * up
            hid[k][c, x] = val.astype(jnp.bfloat16).astype(jnp.float32)
            block = hid[k].at[c, x]
            hx = send(block, block, s_h.at[k, 0], r_h.at[k, 0], x_peer)
            h1 = send(block, block, s_h.at[k, 1], r_h.at[k, 1], core_peer)
            return hx, h1

    def forward(k, hx):
        with jax.named_scope(f"forward{k}"):
            hx.wait_recv()
            block = hid[k].at[c, ox]
            return send(block, block, s_h.at[k, 2], r_h.at[k, 2], core_peer)

    def arrived(k, h1, h2):
        h1.wait_recv()
        h2.wait_recv()

    def half(k, side):
        return hid[k][side].reshape(n_ra * subs[k] // 2, units).astype(jnp.bfloat16)

    def lower(k, h1, h2):
        with jax.named_scope(f"lower{k}"):
            pl.when(c != oy)(functools.partial(arrived, k, h1, h2))
            rows = half(k, oy)
            out = []
            for h, (start, size) in enumerate(slices):
                cols = pl.ds(start, size)
                got = jnp.dot(rows, wd[:, cols], preferred_element_type=jnp.float32)
                dn[k][oy, :, :, cols] = got.reshape(nz, subs[k], size)
                out.append(send(dn[k].at[oy, :, :, cols], yrec[k].at[:, :, cols],
                                s_y.at[k, h], r_y.at[k, h], y_peer))
            pl.when(c == oy)(functools.partial(arrived, k, h1, h2))
            got = jnp.dot(half(k, y), wd[...], preferred_element_type=jnp.float32)
            dn[k][y] = got.reshape(nz, subs[k], depth)
            return out

    def across(k, copies):
        with jax.named_scope(f"across{k}"):
            out = []
            for h, (start, size) in enumerate(slices):
                cols = pl.ds(start, size)
                copies[h].wait_recv()
                dn[k][y, :, :, cols] += yrec[k][:, :, cols]
                for d in range(1, nz):
                    out.append(send(
                        dn[k].at[y, lax.rem(z + d, nz), :, cols], zrec[k].at[d - 1, :, cols],
                        s_z.at[k, h, d - 1], r_z.at[k, h, d - 1], z_peers[d - 1]))
            return out

    def finish(k, copies):
        with jax.named_scope(f"finish{k}"):
            for copy in copies:
                copy.wait_recv()
            got = dn[k][y, z]
            for d in range(nz - 1):
                got = got + zrec[k][d]
            at = pl.ds(base[k], subs[k])
            got = mixed[at, :] + got
            mixed[at, :] = got
            osq[0, at, :] = jnp.broadcast_to(jnp.sum(got * got, axis=1, keepdims=True), (subs[k], LANES))
            return [
                send(osq.at[0, at], osq.at[i + 1, at], s_o.at[k, i], r_o.at[k, i], peer)
                for i, peer in enumerate((core_peer, x_peer, diag_peer))]

    def fill(k):
        xb[k][...] = jnp.concatenate(
            [xs[pl.ds((zz * 2 + yy) * own + base[k], subs[k]), :] for yy in range(2) for zz in range(nz)],
            axis=0).astype(jnp.bfloat16)

    def squares():
        with jax.named_scope("squares"):
            lane = lax.broadcasted_iota(jnp.int32, (own, LANES), 1)
            sqp[...] = jnp.zeros_like(sqp)
            for d in range(n_ra):
                xf = tok[pl.ds(d * own, own), :].astype(jnp.float32)
                sq = jnp.broadcast_to(jnp.sum(xf * xf, axis=1, keepdims=True), (own, LANES))
                for k in range(n):
                    at = ((d % 2) * nz + d // 2) * subs[k]
                    quarter = nz * subs[k] // 2
                    q, off = at // quarter, at % quarter
                    val = jnp.where(lane[:subs[k]] == k, sq[base[k]:base[k] + subs[k]], 0.0)
                    sqp[q // 2, q % 2, pl.ds(off, subs[k]), :] += val
            return send(sqp.at[oc], sqd, s_q.at[0], r_q.at[0], core_peer)

    with jax.named_scope("tokens"):
        for load in early:
            load.wait()
    with jax.named_scope("scale"):
        gain = ng[...].astype(jnp.float32).reshape(1, depth)
        for d in range(n_ra):
            at = pl.ds(d * own, own)
            xs[at, :] = tok[at, :].astype(jnp.float32) * gain
        fill(0)
    with jax.named_scope("enter"):
        pl.semaphore_wait(barrier, len(peers))

    a, b, h1, h2, hx, ys, zs, os = {}, {}, {}, {}, {}, {}, {}, {}
    b[0], b[1], waiting = [], [], []
    for k in range(2):
        for p, (start, size) in enumerate(pieces):
            if k == 0:
                with jax.named_scope("weights"):
                    for load in weights[p]:
                        load.wait()
            project(k, p)
            waiting.append((k, p, to_core(k, pl.ds(start, size), p)))
            if k == 0 and p == 0:
                q1 = squares()
            if len(waiting) > 1:
                kk, pp, copy = waiting.pop(0)
                b[kk].append(combine(kk, copy, *pieces[pp], pp))
            if k == 0 and p == 1:
                with jax.named_scope("share"):
                    q1.wait_recv()
                    sqp[c] += sqd[...]
                    q2 = send(sqp.at[c, ox], sqx, s_q.at[1], r_q.at[1], x_peer)
                fill(1)
    for kk, pp, copy in waiting:
        b[kk].append(combine(kk, copy, *pieces[pp], pp))
    for k in range(2, n):
        fill(k)
    for load in late:
        load.wait()
    mixed[...] = 0.1 * rest[...].astype(jnp.float32)
    for t in range(n + 3):
        if t + 2 < n:
            a[t + 2] = whole(t + 2)
        if t == 0:
            q2.wait_recv()
            inv = lax.rsqrt((sqp[c, x] + sqx[...]) / width + EPS)
        if t < n:
            hx[t], h1[t] = activate(t, b[t], inv)
        if t + 2 < n:
            b[t + 2] = join(t + 2, a[t + 2])
        if 0 <= t - 1 < n:
            h2[t - 1] = forward(t - 1, hx[t - 1])
        if t == n and n > 2:
            zs[n - 3] = across(n - 3, ys[n - 3])
        if 0 <= t - 1 < n:
            ys[t - 1] = lower(t - 1, h1[t - 1], h2[t - 1])
        if t == n and n > 3:
            os[n - 4] = finish(n - 4, zs[n - 4])
        if 0 <= t - 2 < n and t != n - 1:
            zs[t - 2] = across(t - 2, ys[t - 2])
        if 0 <= t - 3 < n and t != n - 1:
            os[t - 3] = finish(t - 3, zs[t - 3])
    with jax.named_scope("norm"):
        for k in range(n):
            for copy in os[k]:
                copy.wait_recv()
        osum = osq[0] + osq[1] + osq[2] + osq[3]
        inv_out = lax.rsqrt(osum / width + EPS)[:, :1]
        out_ref[...] = (mixed[...] * inv_out * og[...].astype(jnp.float32).reshape(1, depth)).astype(out_ref.dtype)
    with jax.named_scope("drain"):
        for copy in sends:
            copy.wait_send()


def column_pieces(total):
    tiles = total // TILE
    cuts = [tiles * i // PIECES * TILE for i in range(PIECES)] + [total]
    return [(lo, hi - lo) for lo, hi in zip(cuts[:-1], cuts[1:])]


def chunk_rows(own):
    unit = own // UNITS
    return [unit * share for share in SHARES]


def fused_body(n_ra, width, tokens, norm_gain, w_gate, w_up, w_down, out_gain):
    count, depth = tokens.shape
    units = w_down.shape[0]
    own = count // n_ra
    subs = chunk_rows(own)
    n, nz = len(subs), n_ra // 2
    f32, bf16 = jnp.float32, jnp.bfloat16
    dma = pltpu.SemaphoreType.DMA
    quarters = [n_ra * sub // 4 for sub in subs]
    most = max(quarters)
    return pl.pallas_call(
        functools.partial(kernel, n_ra, width, subs),
        out_shape=jax.ShapeDtypeStruct((own, depth), bf16),
        in_specs=[pl.BlockSpec(memory_space=pl.ANY)] * 6,
        out_specs=pl.BlockSpec(memory_space=pltpu.VMEM),
        scratch_shapes=[
            pltpu.VMEM((count, depth), bf16),
            pltpu.VMEM((own, depth), bf16),
            pltpu.VMEM((depth,), bf16),
            pltpu.VMEM((depth,), bf16),
            pltpu.VMEM((depth, 2 * units), bf16),
            pltpu.VMEM((units, depth), bf16),
            pltpu.VMEM((count, depth), f32),
            pltpu.VMEM((own, depth), f32),
            pltpu.VMEM((2, 2, most, LANES), f32),
            pltpu.VMEM((2, most, LANES), f32),
            pltpu.VMEM((most, LANES), f32),
            pltpu.VMEM((4, own, LANES), f32),
            *[pltpu.VMEM((n_ra * sub, depth), bf16) for sub in subs],
            *[pltpu.VMEM((2, 2, quarter, 2 * units), f32) for quarter in quarters],
            *[pltpu.VMEM((2, quarter, 2 * units), f32) for quarter in quarters],
            *[pltpu.VMEM((quarter, 2 * units), f32) for quarter in quarters],
            *[pltpu.VMEM((2, 2, quarter, units), f32) for quarter in quarters],
            *[pltpu.VMEM((2, nz, sub, depth), f32) for sub in subs],
            *[pltpu.VMEM((nz, sub, depth), f32) for sub in subs],
            *[pltpu.VMEM((nz - 1, sub, depth), f32) for sub in subs],
            dma((5,)),
            dma((PIECES, 2)),
            *[dma((n, PIECES)) for _ in range(4)],
            *[dma((n, 3)) for _ in range(2)],
            *[dma((n, SLICES)) for _ in range(2)],
            *[dma((n, SLICES, nz - 1)) for _ in range(2)],
            *[dma((n, 3)) for _ in range(2)],
            *[dma((2,)) for _ in range(2)],
        ],
        compiler_params=pltpu.CompilerParams(
            collective_id=0, has_side_effects=True, vmem_limit_bytes=VMEM_BYTES),
    )(tokens, norm_gain, w_gate, w_up, w_down, out_gain)


def solution(mesh):
    n_ra, n_cb = mesh.shape["ra"], mesh.shape["cb"]

    def body(*args):
        tokens, w_down = args[0], args[4]
        count, depth = tokens.shape
        units = w_down.shape[0]
        width = depth * n_cb
        tiled = (
            n_cb == 4 and n_ra % 4 == 0 and n_ra > 2
            and count % (n_ra * UNITS * 8) == 0 and units % LANES == 0 and depth % TILE == 0
            and depth % (SLICES * LANES) == 0)
        if tiled:
            return fused_body(n_ra, width, *args)
        return plain_body(width, *args)

    return jax.shard_map(
        body,
        mesh=mesh,
        in_specs=(P(None, "cb"), P("cb"), P("cb", "ra"), P("cb", "ra"), P("ra", "cb"), P("cb")),
        out_specs=P("ra", "cb"),
        check_vma=False,
    )
```
